32 devices in a mesh: sp: 16 (over z, x, core), tp: 2 (over y).
Axes of the slice: x: 2, y: 2, z: 4, core: 2. Of those that a mesh axis runs over, the one named last changes fastest.
Arguments:
- residual: bfloat16 [4096, 2048], P(('sp', 'tp')), may hold values from -6 to 6
- query_vectors: bfloat16 [4096, 512], P('sp', 'tp'), may hold values from -6 to 6
- key_vectors: bfloat16 [4096, 512], P('sp', 'tp'), may hold values from -6 to 6
- value_vectors: bfloat16 [4096, 512], P('sp', 'tp'), may hold values from -6 to 6
- in_gate: float32 [8, 4096], P('tp', 'sp'), may hold values from -9 to 190
- forget_gate: float32 [8, 4096], P('tp', 'sp'), may hold values from -1 to 12
- documents: int32 [4096], P('sp'), may hold values from 0 to 3, never falling along the last dimension, each value on 1 to 2048 neighbouring positions
- w_out: bfloat16 [512, 2048], P('tp'), may hold values from -0.25 to 0.25
- norm_gain: bfloat16 [2048], replicated, may hold values from 0.099609375 to 1.8984375
- w_up: bfloat16 [2048, 8192], P('sp', 'tp'), may hold values from -0.125 to 0.125
- w_down: bfloat16 [8192, 2048], P('tp', 'sp'), may hold values from -0.0625 to 0.0625
Outputs:
- layer_out: bfloat16 [4096, 2048], P(('sp', 'tp'))
The draws below stay inside these ranges and needn't reach their ends.
Inputs may be any that keep to these rules, and one draw needn't show every extreme that they name: `documents`: document numbers never fall along the positions; every document has 1 to 2048 positions.
All inputs are finite; a program needn't handle non-finite values.
Results may differ from the reference program's by a relative error of at most 0.015.
Values may be sent and summed in bfloat16 or wider, within the bound.
A program may use at most 128 MiB of HBM per device.

```python
import math
import jax
import jax.numpy as jnp
import numpy as np
from jax import lax

D = 2048
MEMORY_HEADS = 8
FF = 8192
SPAN = 128
TOK_DEV = 256
HW = 512
PACKED_TOKENS = 4096
DOCS = 4
DOC_MOST = 2048
N_TP = 2


def draw_in_gate(key, part):
    base_key = jax.random.fold_in(key, 0)
    drawn = jnp.clip(jax.random.normal(base_key, (MEMORY_HEADS, PACKED_TOKENS), jnp.float32), -5.5, 4.5) - 3.5
    return drawn


def draw_forget_gate(key, part):
    shuffle_random_key, gradual_random_key, quick_random_key, block_random_key, jitter_random_key, spike_random_key, dropout_random_key = jax.random.split(key, 7)
    head_order = jax.random.permutation(shuffle_random_key, MEMORY_HEADS)
    slow_count = MEMORY_HEADS // 2
    slow_heads = head_order < slow_count
    slow_rate = math.log(10.0) / DOC_MOST * jax.random.uniform(gradual_random_key, (MEMORY_HEADS,), jnp.float32, 0.3, 1.0)
    fast_rate = 1.0 / jax.random.uniform(quick_random_key, (MEMORY_HEADS,), jnp.float32, 30.0, 100.0)
    head_rate = jnp.where(slow_heads, slow_rate, fast_rate)
    block_factor = jnp.exp(jax.random.uniform(block_random_key, (PACKED_TOKENS // TOK_DEV,), jnp.float32, 0.0, math.log(3.0)))
    position_factor = jnp.repeat(block_factor, TOK_DEV)
    noise_part = jax.random.uniform(jitter_random_key, (MEMORY_HEADS, PACKED_TOKENS), jnp.float32, -1.0, 1.0)
    step_rate = head_rate[:, None] * position_factor[None, :] * jnp.exp(noise_part)
    gate_logits = -jnp.log(jnp.expm1(step_rate))
    spike_positions = jax.random.randint(spike_random_key, (4,), 0, PACKED_TOKENS)
    spike_mask = jnp.any(jnp.arange(PACKED_TOKENS)[:, None] == spike_positions[None, :], axis=1)
    spike_height = jax.random.uniform(dropout_random_key, (MEMORY_HEADS, PACKED_TOKENS), jnp.float32, -0.4, 1.4)
    return jnp.where(spike_mask[None, :], spike_height, gate_logits)


def shard_levels(key, shape, cuts, least, largest):
    level = 1.0
    for position, shards_of in cuts:
        heights = jax.random.uniform(jax.random.fold_in(jax.random.fold_in(key, 6), position), (shards_of,), jnp.float32, least / len(cuts), largest / len(cuts))
        level = level * jnp.repeat(jnp.exp(heights), shape[position] // shards_of).reshape((-1,) + (1,) * (len(shape) - 1 - position))
    return level


def length_profile(amount, total, limit, skew):
    loads = [(1 << 20) // math.isqrt(rank ** skew) + 1 for rank in range(2, amount + 1)]
    rest, given = total - limit - (amount - 1), [1] * (amount - 1)
    while rest > 0:
        free = [i for i in range(amount - 1) if given[i] < limit]
        pool, remaining = sum([loads[i] for i in free]), rest
        for i in free:
            more = min(limit - given[i], max(1, remaining * loads[i] // pool), rest)
            given[i] = given[i] + more
            rest = rest - more
    return np.array([limit] + given)


def ragged_sizes(own_key, count, total, most, lean):
    if count == 2:
        one = jax.random.randint(own_key, (), max(1, total - most), min(most, total - 1) + 1)
        return jnp.stack([one, total - one])
    lengths = jnp.asarray(length_profile(count, total, most, lean), jnp.int32)
    twos = (count - 1) // 2
    donor, receiver = lengths[1:1 + 2 * twos:2], lengths[2:2 + 2 * twos:2]
    margin = jnp.minimum(donor - 1, most - receiver)
    moved = jax.random.randint(jax.random.fold_in(own_key, 1), (twos,), 0, 1 << 20) % (margin + 1)
    lengths = lengths.at[1:1 + 2 * twos:2].set(donor - moved).at[2:2 + 2 * twos:2].set(receiver + moved)
    return lengths[jax.random.permutation(jax.random.fold_in(own_key, 2), count)]


def gaussian(rng, dims, width, most, pieces=(), held_as=jnp.bfloat16):
    values = width * jax.random.normal(rng, dims, jnp.float32)
    if pieces:
        values = values * shard_levels(rng, dims, pieces, -0.22, 0.18)
    return jnp.clip(values, -most, most).astype(held_as)


def setup_inputs(seed: int = 0) -> dict:
    arg_keys = jax.random.split(jax.random.key(seed), 12)
    residual = gaussian(arg_keys[0], (PACKED_TOKENS, D), 1.0, 6.0, ((0, 32),))
    query_vectors = gaussian(arg_keys[1], (PACKED_TOKENS, HW), 1.0, 6.0, ((0, 16), (1, 2)))
    key_vectors = gaussian(arg_keys[2], (PACKED_TOKENS, HW), 1.0, 6.0, ((0, 16), (1, 2)))
    value_vectors = gaussian(arg_keys[3], (PACKED_TOKENS, HW), 1.0, 6.0, ((0, 16), (1, 2)))
    in_gate = draw_in_gate(jax.random.fold_in(arg_keys[11], 71), 0)
    forget_gate = draw_forget_gate(jax.random.fold_in(arg_keys[11], 71), 0)
    documents = jnp.searchsorted(jnp.cumsum(ragged_sizes(arg_keys[6], DOCS, PACKED_TOKENS, DOC_MOST, 0)), jnp.arange(PACKED_TOKENS), side="right").astype(jnp.int32)
    w_out = gaussian(arg_keys[7], (HW, D), HW ** -0.5, 0.25, ((0, 2),))
    norm_gain = jnp.clip(1.0 + 0.18 * jax.random.normal(arg_keys[8], (D,), jnp.float32), 0.099609375, 1.8984375).astype(jnp.bfloat16)
    w_up = gaussian(arg_keys[9], (D, FF), D ** -0.5, 0.125, ((0, 16), (1, 2)))
    w_down = gaussian(arg_keys[10], (FF, D), FF ** -0.5, 0.0625, ((0, 2), (1, 16)))
    return {"residual": residual, "query_vectors": query_vectors, "key_vectors": key_vectors, "value_vectors": value_vectors, "in_gate": in_gate, "forget_gate": forget_gate, "documents": documents, "w_out": w_out, "norm_gain": norm_gain, "w_up": w_up, "w_down": w_down}


very_negative = -1e+30
epsilon = 1e-06

def identity_state(head_count, head_dim):
    return (jnp.zeros((head_count, head_dim, head_dim), jnp.float32), jnp.zeros((head_count, head_dim), jnp.float32), jnp.full((head_count,), very_negative, jnp.float32), jnp.zeros((head_count,), jnp.float32), jnp.array(-1.0, jnp.float32), jnp.array(-1.0, jnp.float32))

def combine(earlier, later):
    memory_one, normal_one, top_one, decay_one, first_one, last_one = earlier
    memory_two, normal_two, top_two, decay_two, first_two, last_two = later
    later_empty = first_two < 0.0
    earlier_empty = first_one < 0.0
    keep = later_empty | (first_two == last_two) & (first_two == last_one)
    decay_step = jnp.where(later_empty, 0.0, decay_two)
    top_new = jnp.where(keep, jnp.maximum(decay_step + top_one, top_two), top_two)
    scale_old = jnp.where(keep, jnp.exp(decay_step + top_one - top_new), 0.0)
    scale_new = jnp.exp(top_two - top_new)
    memory_new = scale_old[:, None, None] * memory_one + scale_new[:, None, None] * memory_two
    normal_new = scale_old[:, None] * normal_one + scale_new[:, None] * normal_two
    decay_new = jnp.where(keep, decay_one + decay_step, decay_two)
    first_new = jnp.where(earlier_empty, first_two, first_one)
    last_new = jnp.where(later_empty, last_one, last_two)
    return (memory_new, normal_new, top_new, decay_new, first_new, last_new)

def block_summary(key_block, value_block, gate_block, decay_block, segment):
    cumulative = jnp.cumsum(decay_block, axis=-1)
    latest = segment == segment[-1]
    growth = jnp.where(latest[None, :], cumulative[:, -1:] - cumulative + gate_block, very_negative)
    top_log = lax.optimization_barrier(jnp.max(growth, axis=-1))
    weight_table = jnp.exp(growth - top_log[:, None])
    key_expanded = key_block.astype(jnp.float32)
    value_expanded = value_block.astype(jnp.float32)
    memory_matrix = jnp.einsum('jw,wjm,wju->jmu', weight_table, key_expanded, value_expanded, precision=lax.Precision.HIGHEST)
    normal = jnp.einsum('hs,shk->hk', weight_table, key_expanded, precision=lax.Precision.HIGHEST)
    return (memory_matrix, normal, top_log, cumulative[:, -1], segment[0], segment[-1])

def block_output(query_block, key_block, value_block, gate_block, decay_block, segment, state):
    memory_matrix, normal, top_log, total_decay, first_doc, last_doc = state
    head_dim = query_block.shape[2]
    length = segment.shape[0]
    cumulative = jnp.cumsum(decay_block, axis=-1)
    row_ids = lax.broadcasted_iota(jnp.int32, (length, length), 0)
    col_ids = lax.broadcasted_iota(jnp.int32, (length, length), 1)
    allowed = (col_ids <= row_ids) & (segment[:, None] == segment[None, :])
    inside = jnp.where(allowed[None], cumulative[:, :, None] - cumulative[:, None, :] + gate_block[:, None, :], very_negative)
    outside = jnp.where((segment == last_doc)[None, :], cumulative + top_log[:, None], very_negative)
    peak_log = jnp.maximum(outside, lax.optimization_barrier(jnp.max(inside, axis=-1)))
    carried = jnp.exp(outside - peak_log)
    scaled_expanded = query_block.astype(jnp.float32) * head_dim ** (-0.5)
    scores = jnp.einsum('lhd,shd->hls', scaled_expanded, key_block.astype(jnp.float32))
    weight_table = jnp.exp(inside - peak_log[:, :, None]) * scores
    rounded = lax.optimization_barrier(weight_table.astype(jnp.bfloat16))
    from_block = jnp.einsum('hls,shv->hlv', rounded.astype(jnp.float32), value_block.astype(jnp.float32))
    memory_readout = jnp.einsum('pug,uga->upa', scaled_expanded, memory_matrix, precision=lax.Precision.HIGHEST)
    numer_part = carried[:, :, None] * memory_readout + from_block
    denom_part = carried * jnp.einsum('lhk,hk->hl', scaled_expanded, normal, precision=lax.Precision.HIGHEST) + lax.optimization_barrier(jnp.sum(weight_table, axis=-1))
    result = numer_part / jnp.maximum(jnp.abs(denom_part), jnp.exp(-peak_log))[:, :, None]
    return jnp.transpose(result, (1, 0, 2)).reshape(length, -1).astype(jnp.bfloat16)

def reference(residual, query_vectors, key_vectors, value_vectors, in_gate, forget_gate, documents, w_out, norm_gain, w_up, w_down):
    head_count = in_gate.shape[0]
    head_dim = query_vectors.shape[1] // head_count
    total_rows = query_vectors.shape[0]
    block_count = total_rows // SPAN

    def to_blocks(vectors):
        return vectors.reshape(block_count, SPAN, head_count, head_dim)

    def gate_blocks(gates):
        return jnp.transpose(gates.reshape(head_count, block_count, SPAN), (1, 0, 2))
    segments = documents.astype(jnp.float32).reshape(block_count, SPAN)
    inputs_all = (to_blocks(query_vectors), to_blocks(key_vectors), to_blocks(value_vectors), gate_blocks(in_gate), gate_blocks(jax.nn.log_sigmoid(forget_gate)), segments)

    def block_step(state, inputs):
        query_block, key_block, value_block, gate_block, decay_block, segment = inputs
        output = block_output(query_block, key_block, value_block, gate_block, decay_block, segment, state)
        summary = block_summary(key_block, value_block, gate_block, decay_block, segment)
        return (combine(state, summary), output)
    _, mixed = lax.scan(block_step, identity_state(head_count, head_dim), inputs_all)
    mixed = mixed.reshape(total_rows, head_count * head_dim)
    group_width = w_up.shape[1] // N_TP

    def row_block(inputs):
        mixed_rows, residual_rows = inputs
        projected = jnp.dot(mixed_rows, w_out, preferred_element_type=jnp.float32)
        middle = (residual_rows.astype(jnp.float32) + projected).astype(jnp.bfloat16)
        middle_wide = middle.astype(jnp.float32)
        factor = lax.rsqrt(lax.optimization_barrier(jnp.mean(middle_wide * middle_wide, axis=-1, keepdims=True)) + epsilon)
        normed = (middle_wide * factor * norm_gain.astype(jnp.float32)).astype(jnp.bfloat16)
        lifted = jnp.dot(normed, w_up, preferred_element_type=jnp.float32)
        hidden = jnp.square(jax.nn.relu(lifted)).astype(jnp.bfloat16)
        summed = jnp.zeros(middle.shape, jnp.float32)
        for column_group in range(N_TP):
            lower = column_group * group_width
            partial_sum = jnp.dot(hidden[:, lower:lower + group_width], w_down[lower:lower + group_width], preferred_element_type=jnp.float32)
            rounded = lax.optimization_barrier(partial_sum.astype(jnp.bfloat16))
            summed = summed + rounded.astype(jnp.float32)
        return (middle_wide + summed).astype(jnp.bfloat16)
    blocks_out = lax.map(row_block, (mixed.reshape(-1, TOK_DEV, head_count * head_dim), residual.reshape(-1, TOK_DEV, residual.shape[1])))
    return blocks_out.reshape(residual.shape)
```

```python
import jax
import jax.numpy as jnp
import numpy as np
from jax import lax
from jax.sharding import Mesh, PartitionSpec as P

DOC_MOST = 2048
very_negative = -1e30
epsilon = 1e-06
SP = ("z", "g")


def combine(earlier, later):
    memory_one, top_one, decay_one, first_one, last_one = earlier
    memory_two, top_two, decay_two, first_two, last_two = later
    later_empty = first_two < 0.0
    earlier_empty = first_one < 0.0
    keep = later_empty | (first_two == last_two) & (first_two == last_one)
    decay_step = jnp.where(later_empty, 0.0, decay_two)
    top_new = jnp.where(keep, jnp.maximum(decay_step + top_one, top_two), top_two)
    scale_old = jnp.where(keep, jnp.exp(decay_step + top_one - top_new), 0.0)
    scale_new = jnp.exp(top_two - top_new)
    memory_new = scale_old[:, None, None] * memory_one + scale_new[:, None, None] * memory_two
    decay_new = jnp.where(keep, decay_one + decay_step, decay_two)
    first_new = jnp.where(earlier_empty, first_two, first_one)
    last_new = jnp.where(later_empty, last_one, last_two)
    return (memory_new, top_new, decay_new, first_new, last_new)


def pack(state):
    memory, top, decay, first, last = state
    heads, _, width = memory.shape
    row = jnp.stack(
        [top, decay, jnp.broadcast_to(first, top.shape), jnp.broadcast_to(last, top.shape)], axis=1
    )
    row = jnp.pad(row, ((0, 0), (0, width - 4)))
    return jnp.concatenate(
        [memory, row[:, None, :], jnp.zeros((heads, 6, width), jnp.float32)], axis=1
    )


def unpack(packed, present):
    rows = packed.shape[1] - 7
    row = packed[:, rows]
    memory = jnp.where(present, packed[:, :rows], 0.0)
    top = jnp.where(present, row[:, 0], very_negative)
    decay = jnp.where(present, row[:, 1], 0.0)
    first = jnp.where(present, row[0, 2], -1.0)
    last = jnp.where(present, row[0, 3], -1.0)
    return (memory, top, decay, first, last)


def shifted(state, distance, length, here):
    packed = lax.ppermute(pack(state), SP, [(i, i + distance) for i in range(length - distance)])
    return unpack(packed, here >= distance)


def on_device(
    residual,
    query_vectors,
    key_vectors,
    value_vectors,
    in_gate,
    forget_gate,
    documents,
    w_out,
    norm_gain,
    w_up,
    w_down,
):
    tok_rows = query_vectors.shape[0]
    heads = in_gate.shape[0]
    head_dim = query_vectors.shape[1] // heads
    length = lax.axis_size(SP)
    here = lax.axis_index(SP)
    tp = lax.axis_size("tp")
    me = lax.axis_index("tp")

    up_part = lax.all_to_all(w_up, "g", split_axis=1, concat_axis=0, tiled=True)
    down_part = lax.all_to_all(w_down, "g", split_axis=0, concat_axis=1, tiled=True)
    up_all = lax.all_gather(up_part, "z", axis=0, tiled=True)

    def turn(value, d):
        return lax.ppermute(value, "tp", [(i, (i + d) % tp) for i in range(tp)])

    w_out_parts = [w_out] + [turn(w_out, d) for d in range(1, tp)]

    segment = documents.astype(jnp.float32)
    decay_log = jax.nn.log_sigmoid(forget_gate)
    cumulative = jnp.cumsum(decay_log, axis=-1)
    key_heads = jnp.transpose(key_vectors.reshape(tok_rows, heads, head_dim), (1, 0, 2))
    value_heads = jnp.transpose(value_vectors.reshape(tok_rows, heads, head_dim), (1, 0, 2))
    query_heads = jnp.transpose(query_vectors.reshape(tok_rows, heads, head_dim), (1, 0, 2))
    query_heads = query_heads * jnp.asarray(head_dim ** (-0.5), query_heads.dtype)
    latest = segment == segment[-1]
    growth = jnp.where(latest[None, :], cumulative[:, -1:] - cumulative + in_gate, very_negative)
    top_log = jnp.max(growth, axis=-1)
    summary_weight = jnp.exp(growth - top_log[:, None])
    key_wide = key_heads.astype(jnp.float32)
    weighted = key_wide * summary_weight[:, :, None]
    memory = jnp.einsum(
        "hsv,hsk->hvk", value_heads.astype(jnp.float32), weighted, precision=lax.Precision.HIGHEST
    )
    normal = jnp.sum(weighted, axis=1)
    state = (
        jnp.concatenate([memory, normal[:, None, :]], axis=1),
        top_log,
        cumulative[:, -1],
        segment[0],
        segment[-1],
    )

    reach = min(length - 1, -(-(DOC_MOST - 1) // tok_rows))
    span = 1
    while span < reach:
        state = combine(shifted(state, span, length, here), state)
        span *= 2
    incoming = shifted(state, 1, length, here)
    memory_in, top_in, _, _, last_in = incoming

    row_ids = lax.broadcasted_iota(jnp.int32, (tok_rows, tok_rows), 0)
    col_ids = lax.broadcasted_iota(jnp.int32, (tok_rows, tok_rows), 1)
    allowed = (col_ids <= row_ids) & (segment[:, None] == segment[None, :])
    inside = jnp.where(
        allowed[None],
        cumulative[:, :, None] - cumulative[:, None, :] + in_gate[:, None, :],
        very_negative,
    )
    peak_inside = jnp.max(inside, axis=-1)
    scores = jnp.einsum(
        "hld,hsd->hls", query_heads, key_heads, preferred_element_type=jnp.float32
    )
    weight_inside = jnp.exp(inside - peak_inside[:, :, None]) * scores
    from_block = jnp.einsum(
        "hls,hsv->hlv",
        weight_inside.astype(jnp.bfloat16),
        value_heads,
        preferred_element_type=jnp.float32,
    )
    sum_inside = jnp.sum(weight_inside, axis=-1)

    outside = jnp.where((segment == last_in)[None, :], cumulative + top_in[:, None], very_negative)
    peak_log = jnp.maximum(outside, peak_inside)
    carried = jnp.exp(outside - peak_log)
    local = jnp.exp(peak_inside - peak_log)
    readout = jnp.einsum(
        "hlk,hvk->hlv",
        query_heads.astype(jnp.float32),
        memory_in,
        precision=lax.Precision.HIGHEST,
    )
    numer = carried[:, :, None] * readout[:, :, :head_dim] + local[:, :, None] * from_block
    denom = carried * readout[:, :, head_dim] + local * sum_inside
    mixed = numer / jnp.maximum(jnp.abs(denom), jnp.exp(-peak_log))[:, :, None]
    mixed = jnp.transpose(mixed, (1, 0, 2)).reshape(tok_rows, -1).astype(jnp.bfloat16)

    own_rows = tok_rows // tp
    mixed_rows = mixed.reshape(tp, own_rows, -1)
    projected = 0.0
    for d in range(tp):
        piece = lax.dynamic_index_in_dim(mixed_rows, (me + d) % tp, 0, keepdims=False)
        if d:
            piece = turn(piece, d)
        projected = projected + jnp.dot(
            piece, w_out_parts[d], preferred_element_type=jnp.float32
        )
    middle = (residual.astype(jnp.float32) + projected).astype(jnp.bfloat16)
    middle_wide = middle.astype(jnp.float32)
    factor = lax.rsqrt(jnp.mean(middle_wide * middle_wide, axis=-1, keepdims=True) + epsilon)
    normed = (middle_wide * factor * norm_gain.astype(jnp.float32)).astype(jnp.bfloat16)

    gathered = lax.all_gather(normed, ("g", "tp"), axis=0, tiled=True)
    down_all = lax.all_gather(down_part, "z", axis=1, tiled=True)
    lifted = jnp.dot(gathered, up_all, preferred_element_type=jnp.float32)
    hidden = jnp.square(jax.nn.relu(lifted)).astype(jnp.bfloat16)
    terms = jnp.dot(hidden, down_all, preferred_element_type=jnp.float32)
    summed = lax.psum_scatter(
        terms.astype(jnp.bfloat16), ("g", "tp"), scatter_dimension=0, tiled=True
    ).astype(jnp.float32)
    return (middle_wide + summed).astype(jnp.bfloat16)


def solution(mesh):
    sp, tp = mesh.shape["sp"], mesh.shape["tp"]
    plane = min(sp, 2 * tp)
    if sp % plane:
        plane = 1
    split = Mesh(np.asarray(mesh.devices).reshape(sp // plane, plane, tp), ("z", "g", "tp"))
    placed = (
        P(("z", "g", "tp"), None),
        P(SP, "tp"),
        P(SP, "tp"),
        P(SP, "tp"),
        P("tp", SP),
        P("tp", SP),
        P(SP),
        P("tp", None),
        P(),
        P(SP, "tp"),
        P("tp", SP),
    )
    return jax.shard_map(
        on_device,
        mesh=split,
        in_specs=placed,
        out_specs=P(("z", "g", "tp"), None),
        check_vma=False,
    )
```

```python
import jax
import jax.numpy as jnp
import numpy as np
from jax import lax
from jax.sharding import Mesh, PartitionSpec as P

DOC_MOST = 2048
very_negative = -1e30
epsilon = 1e-06
SP = ("z", "x", "c")
G = ("x", "c")


def combine(earlier, later):
    memory_one, top_one, decay_one, first_one, last_one = earlier
    memory_two, top_two, decay_two, first_two, last_two = later
    later_empty = first_two < 0.0
    earlier_empty = first_one < 0.0
    keep = later_empty | (first_two == last_two) & (first_two == last_one)
    decay_step = jnp.where(later_empty, 0.0, decay_two)
    top_new = jnp.where(keep, jnp.maximum(decay_step + top_one, top_two), top_two)
    scale_old = jnp.where(keep, jnp.exp(decay_step + top_one - top_new), 0.0)
    scale_new = jnp.exp(top_two - top_new)
    memory_new = scale_old[:, None, None] * memory_one + scale_new[:, None, None] * memory_two
    decay_new = jnp.where(keep, decay_one + decay_step, decay_two)
    first_new = jnp.where(earlier_empty, first_two, first_one)
    last_new = jnp.where(later_empty, last_one, last_two)
    return (memory_new, top_new, decay_new, first_new, last_new)


def pack(state):
    memory, top, decay, first, last = state
    heads, _, width = memory.shape
    row = jnp.stack(
        [top, decay, jnp.broadcast_to(first, top.shape), jnp.broadcast_to(last, top.shape)], axis=1
    )
    row = jnp.pad(row, ((0, 0), (0, width - 4)))
    return jnp.concatenate(
        [memory, row[:, None, :], jnp.zeros((heads, 6, width), jnp.float32)], axis=1
    )


def unpack(packed, present):
    rows = packed.shape[1] - 7
    row = packed[:, rows]
    memory = jnp.where(present, packed[:, :rows], 0.0)
    top = jnp.where(present, row[:, 0], very_negative)
    decay = jnp.where(present, row[:, 1], 0.0)
    first = jnp.where(present, row[0, 2], -1.0)
    last = jnp.where(present, row[0, 3], -1.0)
    return (memory, top, decay, first, last)


def shifted(state, distance, length, here):
    packed = lax.ppermute(pack(state), SP, [(i, i + distance) for i in range(length - distance)])
    return unpack(packed, here >= distance)


def turn(value, axis, d):
    n = lax.axis_size(axis)
    return lax.ppermute(value, axis, [(i, (i + d) % n) for i in range(n)])


def reduced(terms, dim, axis):
    def block(d):
        return lax.index_in_dim(terms, d, dim, keepdims=False)

    total = block(0).astype(jnp.float32)
    for d in range(1, lax.axis_size(axis)):
        total = total + turn(block(d), axis, -d).astype(jnp.float32)
    return total.astype(jnp.bfloat16)


def on_device(
    residual,
    query_vectors,
    key_vectors,
    value_vectors,
    in_gate,
    forget_gate,
    documents,
    w_out,
    norm_gain,
    w_up,
    w_down,
):
    tok_rows = query_vectors.shape[0]
    heads = in_gate.shape[0]
    head_dim = query_vectors.shape[1] // heads
    length = lax.axis_size(SP)
    here = lax.axis_index(SP)
    tp = lax.axis_size("tp")
    me = lax.axis_index("tp")

    plane = lax.axis_size(G)
    up_pieces = jnp.transpose(w_up.reshape(w_up.shape[0], plane, -1), (1, 0, 2))
    up_part = lax.all_to_all(up_pieces, G, split_axis=0, concat_axis=0, tiled=True)
    up_part = up_part.reshape(-1, up_part.shape[-1])
    up_part, w_down, w_out, key_vectors, in_gate, forget_gate, documents = (
        lax.optimization_barrier(
            (up_part, w_down, w_out, key_vectors, in_gate, forget_gate, documents)
        )
    )
    down_part = lax.all_to_all(w_down, G, split_axis=0, concat_axis=1, tiled=True)
    up_all = lax.all_gather(up_part, "z", axis=0, tiled=True)
    down_all = lax.all_gather(down_part, "z", axis=1, tiled=True)

    w_out_parts = [w_out] + [turn(w_out, "tp", d) for d in range(1, tp)]

    segment = documents.astype(jnp.float32)
    decay_log = jax.nn.log_sigmoid(forget_gate)
    cumulative = jnp.cumsum(decay_log, axis=-1)
    key_heads = jnp.transpose(key_vectors.reshape(tok_rows, heads, head_dim), (1, 0, 2))
    value_heads = jnp.transpose(value_vectors.reshape(tok_rows, heads, head_dim), (1, 0, 2))
    query_heads = jnp.transpose(query_vectors.reshape(tok_rows, heads, head_dim), (1, 0, 2))
    query_heads = query_heads * jnp.asarray(head_dim ** (-0.5), query_heads.dtype)
    latest = segment == segment[-1]
    growth = jnp.where(latest[None, :], cumulative[:, -1:] - cumulative + in_gate, very_negative)
    top_log = jnp.max(growth, axis=-1)
    summary_weight = jnp.exp(growth - top_log[:, None])
    key_wide = key_heads.astype(jnp.float32)
    weighted = key_wide * summary_weight[:, :, None]
    memory = jnp.einsum(
        "hsv,hsk->hvk", value_heads.astype(jnp.float32), weighted, precision=lax.Precision.HIGHEST
    )
    normal = jnp.sum(weighted, axis=1)
    state = (
        jnp.concatenate([memory, normal[:, None, :]], axis=1),
        top_log,
        cumulative[:, -1],
        segment[0],
        segment[-1],
    )

    reach = min(length - 1, -(-(DOC_MOST - 1) // tok_rows))
    span = 1
    while span < reach:
        state = combine(shifted(state, span, length, here), state)
        span *= 2
    incoming = shifted(state, 1, length, here)
    memory_in, top_in, _, _, last_in = incoming

    row_ids = lax.broadcasted_iota(jnp.int32, (tok_rows, tok_rows), 0)
    col_ids = lax.broadcasted_iota(jnp.int32, (tok_rows, tok_rows), 1)
    allowed = (col_ids <= row_ids) & (segment[:, None] == segment[None, :])
    inside = jnp.where(
        allowed[None],
        cumulative[:, :, None] - cumulative[:, None, :] + in_gate[:, None, :],
        very_negative,
    )
    peak_inside = jnp.max(inside, axis=-1)
    scores = jnp.einsum(
        "hld,hsd->hls", query_heads, key_heads, preferred_element_type=jnp.float32
    )
    weight_inside = jnp.exp(inside - peak_inside[:, :, None]) * scores
    from_block = jnp.einsum(
        "hls,hsv->hlv",
        weight_inside.astype(jnp.bfloat16),
        value_heads,
        preferred_element_type=jnp.float32,
    )
    sum_inside = jnp.sum(weight_inside, axis=-1)

    outside = jnp.where((segment == last_in)[None, :], cumulative + top_in[:, None], very_negative)
    peak_log = jnp.maximum(outside, peak_inside)
    carried = jnp.exp(outside - peak_log)
    local = jnp.exp(peak_inside - peak_log)
    readout = jnp.einsum(
        "hlk,hvk->hlv",
        query_heads.astype(jnp.float32),
        memory_in,
        precision=lax.Precision.HIGHEST,
    )
    numer = carried[:, :, None] * readout[:, :, :head_dim] + local[:, :, None] * from_block
    denom = carried * readout[:, :, head_dim] + local * sum_inside
    mixed = numer / jnp.maximum(jnp.abs(denom), jnp.exp(-peak_log))[:, :, None]
    mixed = jnp.transpose(mixed, (1, 0, 2)).reshape(tok_rows, -1).astype(jnp.bfloat16)

    own_rows = tok_rows // tp
    mixed_rows = mixed.reshape(tp, own_rows, -1)
    projected = 0.0
    for d in range(tp):
        piece = lax.dynamic_index_in_dim(mixed_rows, (me + d) % tp, 0, keepdims=False)
        if d:
            piece = turn(piece, "tp", d)
        projected = projected + jnp.dot(
            piece, w_out_parts[d], preferred_element_type=jnp.float32
        )
    middle = (residual.astype(jnp.float32) + projected).astype(jnp.bfloat16)
    middle_wide = middle.astype(jnp.float32)
    factor = lax.rsqrt(jnp.mean(middle_wide * middle_wide, axis=-1, keepdims=True) + epsilon)
    normed = (middle_wide * factor * norm_gain.astype(jnp.float32)).astype(jnp.bfloat16)

    gathered = normed
    for axis in ("tp", "x", "c"):
        gathered = jnp.concatenate(
            [gathered] + [turn(gathered, axis, d) for d in range(1, lax.axis_size(axis))], axis=0
        )
    lifted = jnp.dot(gathered, up_all, preferred_element_type=jnp.float32)
    hidden = jnp.square(jax.nn.relu(lifted)).astype(jnp.bfloat16)
    sizes = (lax.axis_size("c"), lax.axis_size("x"), tp)
    half = down_all.shape[1] // 2
    summed = []
    for k, order in enumerate((("c", "x", "tp"), ("c", "tp", "x"))):
        terms = jnp.dot(
            hidden, down_all[:, k * half : (k + 1) * half], preferred_element_type=jnp.float32
        )
        terms = terms.astype(jnp.bfloat16).reshape(*sizes, own_rows, half)
        names = ["c", "x", "tp"]
        for axis in order:
            terms = reduced(terms, names.index(axis), axis)
            names.remove(axis)
        summed.append(terms.astype(jnp.float32))
    return (middle_wide + jnp.concatenate(summed, axis=1)).astype(jnp.bfloat16)


def solution(mesh):
    sp, tp = mesh.shape["sp"], mesh.shape["tp"]
    chips = tp if sp % (2 * tp) == 0 else 1
    cores = 2 if sp % 2 == 0 else 1
    shape = (sp // (chips * cores), chips, cores, tp)
    split = Mesh(np.asarray(mesh.devices).reshape(shape), ("z", "x", "c", "tp"))
    placed = (
        P(("z", "x", "c", "tp"), None),
        P(SP, "tp"),
        P(SP, "tp"),
        P(SP, "tp"),
        P("tp", SP),
        P("tp", SP),
        P(SP),
        P("tp", None),
        P(),
        P(SP, "tp"),
        P("tp", SP),
    )
    return jax.shard_map(
        on_device,
        mesh=split,
        in_specs=placed,
        out_specs=P(("z", "x", "c", "tp"), None),
        check_vma=False,
    )
```
